1024 devices in a mesh: grp: 2 (over x), row: 16 (over z), col: 32 (over y, core).
Axes of the slice: x: 2, y: 16, z: 16, core: 2. Of those that a mesh axis runs over, the one named last changes fastest.
The devices are a block of a 4x16x16 slice.
Arguments:
- tokens: bfloat16 [2, 65536, 2048], P('grp', ('row', 'col')), parts along dimension 0, may hold values from -6 to 6
- norm_gain: bfloat16 [2048], replicated, may hold values from 0.099609375 to 1.8984375
- w_in: bfloat16 [2048, 512], replicated, may hold values from -0.125 to 0.125
- w_out: bfloat16 [512, 2048], replicated, may hold values from -0.25 to 0.25
Outputs:
- mixed: bfloat16 [2, 65536, 2048], P('grp', ('row', 'col')), parts along dimension 0
The draws below stay inside these ranges and needn't reach their ends.
There are 2 independent parts, one for each index of `grp`. The reference program is written for one: setup_inputs(seed, part) draws one part's arguments, and reference() takes and returns one part's arrays. A program takes and returns all parts, laid end to end along the dimension named above; an argument that names none is the same for every part. Nothing has to cross between parts.
All inputs are finite; a program needn't handle non-finite values.
Results may differ from the reference program's by a relative error of at most 0.013.
Values may be sent and summed in bfloat16 or wider, within the bound.
No kernel may reach another device: no remote copies, remote signals or barrier semaphores. Data moves between devices by JAX's collectives and lax.ppermute only.
A program may use at most 32 MiB of HBM per device.

```python
import jax
import jax.numpy as jnp
from jax import lax

D = 2048
FEATS = 512
GROUP_CH = 128
SEQS = 1
LENGTH = 65536


def level_of(rng, dims, pieces, low, high):
    factor_of = 1.0
    for dim, shards_of in pieces:
        steps = jax.random.uniform(jax.random.fold_in(jax.random.fold_in(rng, 6), dim), (shards_of,), jnp.float32, low / len(pieces), high / len(pieces))
        factor_of = factor_of * jnp.repeat(jnp.exp(steps), dims[dim] // shards_of).reshape((-1,) + (1,) * (len(dims) - 1 - dim))
    return factor_of


def bell_draw(key, shape, spread, bound, split=(), held_as=jnp.bfloat16):
    factor_of = level_of(key, shape, split, -0.22, 0.18) if split else 1.0
    result = jax.random.normal(key, shape, jnp.float32) * spread * factor_of
    return jnp.minimum(jnp.maximum(result, -bound), bound).astype(held_as)


def setup_inputs(seed: int = 0, part: int = 0) -> dict:
    key_of = jax.random.split(jax.random.key(seed), 5)
    part_splits = jax.random.split(jax.random.fold_in(key_of[4], part), 5)
    tokens = bell_draw(part_splits[0], (SEQS, LENGTH, D), 1.0, 6.0, ((1, 512),))
    norm_gain = jnp.clip(1.0 + 0.18 * jax.random.normal(key_of[1], (D,), jnp.float32), 0.099609375, 1.8984375).astype(jnp.bfloat16)
    w_in = bell_draw(key_of[2], (D, FEATS), D ** -0.5, 0.125)
    w_out = bell_draw(key_of[3], (FEATS, D), FEATS ** -0.5, 0.25)
    return {"tokens": tokens, "norm_gain": norm_gain, "w_in": w_in, "w_out": w_out}


def reference(tokens, norm_gain, w_in, w_out):
    widened = tokens.astype(jnp.float32)
    factor = lax.rsqrt(lax.optimization_barrier(jnp.mean(widened * widened, -1, keepdims=True)) + 1e-06)
    normed = (widened * factor * norm_gain.astype(jnp.float32)).astype(jnp.bfloat16)
    flat = normed.reshape(SEQS * LENGTH, D)
    mixin = jnp.dot(flat, w_in, preferred_element_type=jnp.float32).astype(jnp.bfloat16)
    grouped = mixin.astype(jnp.float32).reshape(SEQS, LENGTH, FEATS // GROUP_CH, GROUP_CH)
    spectrum = jnp.fft.fft2(grouped, axes=(1, 3), norm='ortho').real
    spectrum = spectrum.astype(jnp.float32).reshape(SEQS * LENGTH, FEATS).astype(jnp.bfloat16)
    mixed = jnp.dot(spectrum, w_out, preferred_element_type=jnp.float32).astype(jnp.bfloat16)
    return mixed.reshape(SEQS, LENGTH, D)
```

```python
import functools
import math

import jax
import jax.numpy as jnp
import numpy as np
from jax import lax
from jax.experimental import pallas as pl
from jax.experimental.pallas import tpu as pltpu
from jax.sharding import PartitionSpec as P

GROUP_CH = 128
NORM_EPS = 1e-06
CHUNKS = 4
VMEM_LIMIT = 16 * 1024 * 1024

BF16 = jnp.bfloat16
F32 = jnp.float32


def channel_tables():
    half = GROUP_CH // 2
    q = np.arange(GROUP_CH)[:, None]
    f = np.arange(GROUP_CH)[None, :]
    freq = np.where(f <= half, f, GROUP_CH - f)
    angle = 2.0 * np.pi * (q * freq % GROUP_CH) / GROUP_CH
    spread = np.where(f <= half, np.cos(angle), np.sin(angle))
    merge = np.zeros((GROUP_CH, GROUP_CH))
    merge[0, 0] = merge[half, half] = 1.0
    for m in range(1, half):
        merge[m, m] = merge[m, GROUP_CH - m] = 1.0
        merge[GROUP_CH - m, m] = -1.0
        merge[GROUP_CH - m, GROUP_CH - m] = 1.0
    return spread, merge


def sequence_tables(rows, cols, toks):
    length = rows * cols * toks
    low = 2 * toks
    high = length // low
    assert high == low
    halves = cols // 2
    a = (np.arange(rows)[None, :] * halves + np.arange(halves)[:, None]).reshape(-1)
    k1 = np.arange(high)
    first = 2.0 * np.pi * (a[:, None] * k1[None, :] % high) / high
    b = np.arange(low)
    turn = 2.0 * np.pi * (b[:, None] * k1[None, :] % length) / length
    last = 2.0 * np.pi * (a[:, None] * b[None, :] % low) / low
    scale = 1.0 / math.sqrt(length * GROUP_CH)
    return (
        np.concatenate([np.cos(first), -np.sin(first)], axis=1),
        np.stack([np.cos(turn) * scale, -np.sin(turn) * scale]),
        np.concatenate([np.cos(last), np.sin(last)], axis=1),
    )


def project(tok_hbm, gain_ref, w_hbm, spread_ref, out_ref, tok_v, w_v, sems):
    toks, width = tok_v.shape
    part = width // CHUNKS
    copies = []
    for j in range(CHUNKS):
        at = pl.ds(j * part, part)
        copies.append(
            (
                pltpu.make_async_copy(tok_hbm.at[0, :, at], tok_v.at[:, at], sems.at[0, j]),
                pltpu.make_async_copy(w_hbm.at[at, :], w_v.at[at, :], sems.at[1, j]),
            )
        )
    for pair in copies:
        for copy in pair:
            copy.start()
    squares = jnp.zeros((toks, 1), F32)
    total = jnp.zeros((toks, w_v.shape[1]), F32)
    for j in range(CHUNKS):
        at = pl.ds(j * part, part)
        copies[j][0].wait()
        x = tok_v[:, at].astype(F32)
        squares += jnp.sum(x * x, axis=-1, keepdims=True)
        scaled = (x * gain_ref[:, at].astype(F32)).astype(BF16)
        copies[j][1].wait()
        total += jnp.dot(scaled, w_v[at, :], preferred_element_type=F32)
    factor = lax.rsqrt(squares * (1.0 / width) + NORM_EPS)
    mixin = (total * factor).astype(BF16)
    for g in range(w_v.shape[1] // GROUP_CH):
        at = slice(g * GROUP_CH, (g + 1) * GROUP_CH)
        out_ref[at, :] = lax.dot_general(
            spread_ref[...], mixin[:, at], (((0,), (1,)), ((), ())), preferred_element_type=F32
        ).astype(BF16)


def transform(which_ref, x_ref, first_ref, turn_ref, last_ref, out_ref):
    halves, _, rows, toks = x_ref.shape
    high = first_ref.shape[0]
    sine = which_ref[0] == 1
    parts = []
    for c in range(2):
        x = x_ref[:, c].reshape(halves * rows, toks)
        parts.append(
            lax.dot_general(x, first_ref[...], (((0,), (0,)), ((), ())), preferred_element_type=F32)
        )
    y = jnp.concatenate(parts, axis=0)
    y_re, y_im = y[:, :high], y[:, high:]
    w_re, w_im = turn_ref[0], turn_ref[1]
    u_re = y_re * w_re - y_im * w_im
    u_im = y_re * w_im + y_im * w_re
    both = jnp.concatenate(
        [jnp.where(sine, -u_im, u_re).astype(BF16), jnp.where(sine, u_re, u_im).astype(BF16)],
        axis=0,
    )
    z = jnp.dot(last_ref[...], both, preferred_element_type=F32).astype(BF16)
    for c in range(2):
        out_ref[:, c] = z[:, c * toks : (c + 1) * toks].reshape(halves, rows, toks)


def merge_out(x_ref, merge_ref, w_ref, out_ref):
    feats = x_ref.shape[0]
    pieces = []
    for g in range(feats // GROUP_CH):
        at = slice(g * GROUP_CH, (g + 1) * GROUP_CH)
        pieces.append(
            lax.dot_general(
                x_ref[at, :], merge_ref[...], (((0,), (0,)), ((), ())), preferred_element_type=F32
            ).astype(BF16)
        )
    spectrum = jnp.concatenate(pieces, axis=1)
    out_ref[0] = jnp.dot(spectrum, w_ref[...], preferred_element_type=F32).astype(BF16)


def shards(rows, cols, tokens, norm_gain, w_in, w_out):
    _, toks, width = tokens.shape
    feats = w_in.shape[1]
    halves = cols // 2
    spread, merge = channel_tables()
    first, turn, last = sequence_tables(rows, cols, toks)
    vmem = pl.BlockSpec(memory_space=pltpu.VMEM)
    smem = pl.BlockSpec(memory_space=pltpu.SMEM)
    hbm = pl.BlockSpec(memory_space=pl.ANY)

    feature = lax.axis_index("row") * cols + lax.axis_index("col")
    sine = (feature % GROUP_CH > GROUP_CH // 2).astype(jnp.int32).reshape(1)

    sent = pl.pallas_call(
        project,
        out_shape=jax.ShapeDtypeStruct((feats, toks), BF16),
        in_specs=[hbm, vmem, hbm, vmem],
        out_specs=vmem,
        scratch_shapes=[
            pltpu.VMEM((toks, width), BF16),
            pltpu.VMEM((width, feats), BF16),
            pltpu.SemaphoreType.DMA((2, CHUNKS)),
        ],
        name="project",
    )(tokens, norm_gain.reshape(1, width), w_in, jnp.asarray(spread, BF16))
    sent = lax.all_to_all(
        sent.reshape(rows, cols, toks), "row", split_axis=0, concat_axis=0, tiled=True
    )
    sent = lax.all_to_all(
        sent.transpose(1, 0, 2), "col", split_axis=0, concat_axis=0, tiled=True
    )
    back = pl.pallas_call(
        transform,
        out_shape=jax.ShapeDtypeStruct((halves, 2, rows, toks), BF16),
        in_specs=[smem, vmem, vmem, vmem, vmem],
        out_specs=vmem,
        compiler_params=pltpu.CompilerParams(vmem_limit_bytes=VMEM_LIMIT),
        name="transform",
    )(
        sine,
        sent.reshape(halves, 2, rows, toks),
        jnp.asarray(first, BF16),
        jnp.asarray(turn, F32),
        jnp.asarray(last, BF16),
    )
    back = lax.all_to_all(
        back.reshape(cols, rows, toks), "col", split_axis=0, concat_axis=0, tiled=True
    )
    back = lax.all_to_all(
        back.transpose(1, 0, 2), "row", split_axis=0, concat_axis=0, tiled=True
    )
    return pl.pallas_call(
        merge_out,
        out_shape=jax.ShapeDtypeStruct((1, toks, width), BF16),
        in_specs=[vmem, vmem, vmem],
        out_specs=vmem,
        compiler_params=pltpu.CompilerParams(vmem_limit_bytes=VMEM_LIMIT),
        name="merge_out",
    )(back.reshape(feats, toks), jnp.asarray(merge, BF16), w_out)


def solution(mesh):
    return jax.shard_map(
        functools.partial(shards, mesh.shape["row"], mesh.shape["col"]),
        mesh=mesh,
        in_specs=(P("grp", ("row", "col"), None), P(), P(), P()),
        out_specs=P("grp", ("row", "col"), None),
        check_vma=False,
    )
```

```python
import functools
import math

import jax
import jax.numpy as jnp
import numpy as np
from jax import lax
from jax.experimental import pallas as pl
from jax.experimental.pallas import tpu as pltpu
from jax.sharding import PartitionSpec as P

GROUP_CH = 128
NORM_EPS = 1e-06
CORES = 2
CHUNKS = 4
VMEM_LIMIT = 16 * 1024 * 1024
PROJECT_LIMIT = 60 * 1024 * 1024

BF16 = jnp.bfloat16
F32 = jnp.float32


def channel_tables():
    half = GROUP_CH // 2
    q = np.arange(GROUP_CH)[:, None]
    f = np.arange(GROUP_CH)[None, :]
    freq = np.where(f <= half, f, GROUP_CH - f)
    angle = 2.0 * np.pi * (q * freq % GROUP_CH) / GROUP_CH
    spread = np.where(f <= half, np.cos(angle), np.sin(angle))
    merge = np.zeros((GROUP_CH, GROUP_CH))
    merge[0, 0] = merge[half, half] = 1.0
    for m in range(1, half):
        merge[m, m] = merge[m, GROUP_CH - m] = 1.0
        merge[GROUP_CH - m, m] = -1.0
        merge[GROUP_CH - m, GROUP_CH - m] = 1.0
    return spread, merge


def sequence_tables(rows, chips, toks):
    length = rows * chips * CORES * toks
    low = CORES * toks
    high = rows * chips
    assert high == low
    a = (np.arange(rows)[None, :] * chips + np.arange(chips)[:, None]).reshape(-1)
    k1 = np.arange(high)
    b = np.arange(low)
    first = 2.0 * np.pi * (a[:, None] * k1[None, :] % high) / high
    turn = 2.0 * np.pi * (b[:, None] * k1[None, :] % length) / length
    last = 2.0 * np.pi * (a[:, None] * b[None, :] % low) / low
    scale = 1.0 / math.sqrt(length * GROUP_CH)

    def halves(table):
        return [table[..., h * toks : (h + 1) * toks] for h in range(CORES)]

    first = np.stack([np.concatenate([np.cos(t), -np.sin(t)], axis=1) for t in halves(first)])
    turn = np.stack(
        [
            np.stack([np.stack([np.cos(t), -np.sin(t)]) * scale for t in halves(turn[c * toks : (c + 1) * toks])])
            for c in range(CORES)
        ]
    )
    last = np.stack([np.concatenate([np.cos(t), np.sin(t)], axis=1) for t in halves(last)])
    return first, turn, last


def project(tok_hbm, gain_hbm, w_hbm, spread_hbm, out_ref, tok_v, w_v, gain_v, spread_v, sems, small_sems):
    toks, width = tok_v.shape
    part = width // CHUNKS
    small = [
        pltpu.make_async_copy(gain_hbm, gain_v, small_sems.at[0]),
        pltpu.make_async_copy(spread_hbm, spread_v, small_sems.at[1]),
    ]
    copies = []
    for j in range(CHUNKS):
        at = pl.ds(j * part, part)
        copies.append(
            (
                pltpu.make_async_copy(tok_hbm.at[0, :, at], tok_v.at[:, at], sems.at[0, j]),
                pltpu.make_async_copy(w_hbm.at[at, :], w_v.at[at, :], sems.at[1, j]),
            )
        )
    small[0].start()
    for pair in copies:
        for copy in pair:
            copy.start()
    small[1].start()
    small[0].wait()
    gain = gain_v[...].astype(F32).reshape(1, width)
    squares = jnp.zeros((toks, 1), F32)
    total = jnp.zeros((toks, w_v.shape[1]), F32)
    for j in range(CHUNKS):
        at = slice(j * part, (j + 1) * part)
        copies[j][0].wait()
        x = tok_v[:, at].astype(F32)
        squares += jnp.sum(x * x, axis=-1, keepdims=True)
        scaled = (x * gain[:, at]).astype(BF16)
        copies[j][1].wait()
        total += jnp.dot(scaled, w_v[at, :], preferred_element_type=F32)
    factor = lax.rsqrt(squares * (1.0 / width) + NORM_EPS)
    mixin = (total * factor).astype(BF16)
    small[1].wait()
    for g in range(w_v.shape[1] // GROUP_CH):
        at = slice(g * GROUP_CH, (g + 1) * GROUP_CH)
        out_ref[at, :] = lax.dot_general(
            spread_v[...], mixin[:, at], (((0,), (1,)), ((), ())), preferred_element_type=F32
        ).astype(BF16)


def transform_a(which_ref, x_ref, first_ref, turn_ref, own_ref, send_ref):
    chips, _, rows, toks = x_ref.shape
    core = which_ref[0]
    for half, ref in ((core, own_ref), (1 - core, send_ref)):
        table = first_ref[half]
        w_re, w_im = turn_ref[core, half, 0], turn_ref[core, half, 1]
        for j in range(CORES):
            sine = which_ref[1 + j] == 1
            y = lax.dot_general(
                x_ref[:, j].reshape(chips * rows, toks),
                table,
                (((0,), (0,)), ((), ())),
                preferred_element_type=F32,
            )
            y_re, y_im = y[:, :toks], y[:, toks:]
            u_re = (y_re * w_re - y_im * w_im).astype(BF16)
            u_im = (y_re * w_im + y_im * w_re).astype(BF16)
            at = slice(j * toks, (j + 1) * toks)
            ref[:toks, at] = jnp.where(sine, -u_im, u_re)
            ref[toks:, at] = jnp.where(sine, u_re, u_im)


def transform_b(which_ref, own_ref, got_ref, last_ref, out_ref):
    chips, _, rows, toks = out_ref.shape
    core = which_ref[0]
    z = jnp.dot(last_ref[core], own_ref[...], preferred_element_type=F32)
    z += jnp.dot(last_ref[1 - core], got_ref[...], preferred_element_type=F32)
    z = z.astype(BF16)
    for j in range(CORES):
        out_ref[:, j] = z[:, j * toks : (j + 1) * toks].reshape(chips, rows, toks)


def merge_out(x_ref, merge_ref, w_ref, out_hbm, out_v, sems):
    feats = x_ref.shape[0]
    width = w_ref.shape[1]
    pieces = []
    for g in range(feats // GROUP_CH):
        at = slice(g * GROUP_CH, (g + 1) * GROUP_CH)
        pieces.append(
            lax.dot_general(
                x_ref[at, :], merge_ref[...], (((0,), (0,)), ((), ())), preferred_element_type=F32
            ).astype(BF16)
        )
    spectrum = jnp.concatenate(pieces, axis=1)
    part = width // CHUNKS
    copies = []
    for j in range(CHUNKS):
        at = slice(j * part, (j + 1) * part)
        out_v[:, at] = jnp.dot(spectrum, w_ref[:, at], preferred_element_type=F32).astype(BF16)
        copies.append(
            pltpu.make_async_copy(
                out_v.at[:, pl.ds(j * part, part)],
                out_hbm.at[0, :, pl.ds(j * part, part)],
                sems.at[j],
            )
        )
        copies[-1].start()
    for copy in copies:
        copy.wait()


VMEM = pl.BlockSpec(memory_space=pltpu.VMEM)
SMEM = pl.BlockSpec(memory_space=pltpu.SMEM)
HBM = pl.BlockSpec(memory_space=pltpu.HBM)


def call_project(tokens, norm_gain, w_in, spread):
    _, toks, width = tokens.shape
    feats = w_in.shape[1]
    return pl.pallas_call(
        project,
        out_shape=jax.ShapeDtypeStruct((feats, toks), BF16),
        in_specs=[HBM, HBM, HBM, HBM],
        out_specs=VMEM,
        scratch_shapes=[
            pltpu.VMEM((toks, width), BF16),
            pltpu.VMEM((width, feats), BF16),
            pltpu.VMEM(norm_gain.shape, BF16),
            pltpu.VMEM(spread.shape, BF16),
            pltpu.SemaphoreType.DMA((2, CHUNKS)),
            pltpu.SemaphoreType.DMA((2,)),
        ],
        compiler_params=pltpu.CompilerParams(vmem_limit_bytes=PROJECT_LIMIT),
        name="project",
    )(tokens, norm_gain, w_in, spread)


def call_transform_a(which, x, first, turn):
    toks = x.shape[-1]
    half = jax.ShapeDtypeStruct((2 * toks, CORES * toks), BF16)
    return pl.pallas_call(
        transform_a,
        out_shape=(half, half),
        in_specs=[SMEM, VMEM, VMEM, VMEM],
        out_specs=(VMEM, VMEM),
        compiler_params=pltpu.CompilerParams(vmem_limit_bytes=VMEM_LIMIT),
        name="transform_a",
    )(which, x, first, turn)


def call_transform_b(which, own, got, last, shape):
    return pl.pallas_call(
        transform_b,
        out_shape=jax.ShapeDtypeStruct(shape, BF16),
        in_specs=[SMEM, VMEM, VMEM, VMEM],
        out_specs=VMEM,
        compiler_params=pltpu.CompilerParams(vmem_limit_bytes=VMEM_LIMIT),
        name="transform_b",
    )(which, own, got, last)


def call_merge_out(x, merge, w_out):
    width = w_out.shape[1]
    toks = x.shape[1]
    return pl.pallas_call(
        merge_out,
        out_shape=jax.ShapeDtypeStruct((1, toks, width), BF16),
        in_specs=[VMEM, VMEM, VMEM],
        out_specs=HBM,
        scratch_shapes=[pltpu.VMEM((toks, width), BF16), pltpu.SemaphoreType.DMA((CHUNKS,))],
        compiler_params=pltpu.CompilerParams(vmem_limit_bytes=VMEM_LIMIT),
        name="merge_out",
    )(x, merge, w_out)


def shards(rows, cols, tokens, norm_gain, w_in, w_out):
    _, toks, width = tokens.shape
    feats = w_in.shape[1]
    chips = cols // CORES
    spread, merge = channel_tables()
    first, turn, last = sequence_tables(rows, chips, toks)
    lines = [[CORES * y + c for y in range(chips)] for c in range(CORES)]
    pairs = [(i, i ^ 1) for i in range(cols)]

    col = lax.axis_index("col")
    core = col % CORES
    feature = lax.axis_index("row") * cols + (col - core)
    which = jnp.stack(
        [core] + [((feature + j) % GROUP_CH > GROUP_CH // 2).astype(jnp.int32) for j in range(CORES)]
    )
    which, tokens = lax.optimization_barrier((which, tokens))

    def along_row(x):
        return lax.all_to_all(x, "row", split_axis=0, concat_axis=0, tiled=True)

    def along_line(x):
        return lax.all_to_all(
            x, "col", split_axis=0, concat_axis=0, tiled=True, axis_index_groups=lines
        )

    sent = call_project(tokens, norm_gain, w_in, jnp.asarray(spread, BF16))
    sent = along_row(sent.reshape(rows, cols, toks))
    sent = along_line(sent.transpose(1, 0, 2))
    shape = (chips, CORES, rows, toks)
    own, give = call_transform_a(
        which, sent.reshape(shape), jnp.asarray(first, BF16), jnp.asarray(turn, F32)
    )
    got = lax.ppermute(give, "col", pairs)
    back = call_transform_b(which, own, got, jnp.asarray(last, BF16), shape)
    back = along_line(back.reshape(cols, rows, toks))
    back = along_row(back.transpose(1, 0, 2))
    return call_merge_out(back.reshape(feats, toks), jnp.asarray(merge, BF16), w_out)


def solution(mesh):
    return jax.shard_map(
        functools.partial(shards, mesh.shape["row"], mesh.shape["col"]),
        mesh=mesh,
        in_specs=(P("grp", ("row", "col"), None), P(), P(), P()),
        out_specs=P("grp", ("row", "col"), None),
        check_vma=False,
    )
```

```python
import functools
import math

import jax
import jax.numpy as jnp
import numpy as np
from jax import lax
from jax.experimental import pallas as pl
from jax.experimental.pallas import tpu as pltpu
from jax.sharding import PartitionSpec as P

GROUP_CH = 128
NORM_EPS = 1e-06
CORES = 2
CHUNKS = 4
VMEM_LIMIT = 16 * 1024 * 1024
PROJECT_LIMIT = 60 * 1024 * 1024

BF16 = jnp.bfloat16
F32 = jnp.float32


def channel_tables():
    half = GROUP_CH // 2
    q = np.arange(GROUP_CH)[:, None]
    f = np.arange(GROUP_CH)[None, :]
    freq = np.where(f <= half, f, GROUP_CH - f)
    angle = 2.0 * np.pi * (q * freq % GROUP_CH) / GROUP_CH
    spread = np.where(f <= half, np.cos(angle), np.sin(angle))
    merge = np.zeros((GROUP_CH, GROUP_CH))
    merge[0, 0] = merge[half, half] = 1.0
    for m in range(1, half):
        merge[m, m] = merge[m, GROUP_CH - m] = 1.0
        merge[GROUP_CH - m, m] = -1.0
        merge[GROUP_CH - m, GROUP_CH - m] = 1.0
    return spread, merge


def sequence_tables(rows, chips, toks):
    length = rows * chips * CORES * toks
    low = CORES * toks
    high = rows * chips
    assert high == low
    a = (np.arange(rows)[None, :] * chips + np.arange(chips)[:, None]).reshape(-1)
    k1 = np.arange(high)
    b = np.arange(low)
    first = 2.0 * np.pi * (a[:, None] * k1[None, :] % high) / high
    turn = 2.0 * np.pi * (b[:, None] * k1[None, :] % length) / length
    last = 2.0 * np.pi * (a[:, None] * b[None, :] % low) / low
    scale = 1.0 / math.sqrt(length * GROUP_CH)

    def halves(table):
        return [table[..., h * toks : (h + 1) * toks] for h in range(CORES)]

    first = np.concatenate([f(t) for t in halves(first) for f in (np.cos, lambda v: -np.sin(v))], axis=1)
    turn = np.stack(
        [
            np.stack([np.stack([np.cos(t), -np.sin(t)]) * scale for t in halves(turn[c * toks : (c + 1) * toks])])
            for c in range(CORES)
        ]
    )
    last = np.stack([np.concatenate([np.cos(t), np.sin(t)], axis=1) for t in halves(last)])
    return first, turn, last


def project(
    tok_hbm, gain_hbm, w_hbm, spread_hbm, out_hbm, tok_v, w_v, gain_v, spread_v, out_v, sems, small_sems, out_sems
):
    toks, width = tok_v.shape
    part = width // CHUNKS
    small = [
        pltpu.make_async_copy(gain_hbm, gain_v, small_sems.at[0]),
        pltpu.make_async_copy(spread_hbm, spread_v, small_sems.at[1]),
    ]
    copies = []
    for j in range(CHUNKS):
        at = pl.ds(j * part, part)
        copies.append(
            (
                pltpu.make_async_copy(tok_hbm.at[0, :, at], tok_v.at[:, at], sems.at[0, j]),
                pltpu.make_async_copy(w_hbm.at[at, :], w_v.at[at, :], sems.at[1, j]),
            )
        )
    small[0].start()
    for pair in copies:
        for copy in pair:
            copy.start()
    small[1].start()
    small[0].wait()
    gain = gain_v[...].astype(F32).reshape(1, width)
    squares = jnp.zeros((toks, 1), F32)
    total = jnp.zeros((toks, w_v.shape[1]), F32)
    for j in range(CHUNKS):
        at = slice(j * part, (j + 1) * part)
        copies[j][0].wait()
        x = tok_v[:, at].astype(F32)
        squares += jnp.sum(x * x, axis=-1, keepdims=True)
        scaled = (x * gain[:, at]).astype(BF16)
        copies[j][1].wait()
        total += jnp.dot(scaled, w_v[at, :], preferred_element_type=F32)
    factor = lax.rsqrt(squares * (1.0 / width) + NORM_EPS)
    mixin = (total * factor).astype(BF16)
    small[1].wait()
    leaving = []
    for g in range(w_v.shape[1] // GROUP_CH):
        at = slice(g * GROUP_CH, (g + 1) * GROUP_CH)
        out_v[at, :] = lax.dot_general(
            spread_v[...], mixin[:, at], (((0,), (1,)), ((), ())), preferred_element_type=F32
        ).astype(BF16)
        rows = pl.ds(g * GROUP_CH, GROUP_CH)
        leaving.append(pltpu.make_async_copy(out_v.at[rows, :], out_hbm.at[rows, :], out_sems.at[g]))
        leaving[-1].start()
    for copy in leaving:
        copy.wait()


def transform_a(x_ref, first_ref, turn_ref, own_ref, send_ref):
    chips, _, rows, toks = x_ref.shape
    cols = chips * CORES
    col = lax.axis_index("col")
    core = lax.rem(col, CORES)
    feature = lax.axis_index("row") * cols + (col - core)
    low = core == 0
    for j in range(CORES):
        sine = lax.rem(feature + j, GROUP_CH) > GROUP_CH // 2
        y = lax.dot_general(
            x_ref[:, j].reshape(chips * rows, toks),
            first_ref[...],
            (((0,), (0,)), ((), ())),
            preferred_element_type=F32,
        )
        halves = []
        for h in range(CORES):
            y_re = y[:, 2 * h * toks : (2 * h + 1) * toks]
            y_im = y[:, (2 * h + 1) * toks : (2 * h + 2) * toks]
            w_re, w_im = turn_ref[core, h, 0], turn_ref[core, h, 1]
            u_re = (y_re * w_re - y_im * w_im).astype(BF16)
            u_im = (y_re * w_im + y_im * w_re).astype(BF16)
            halves.append((jnp.where(sine, -u_im, u_re), jnp.where(sine, u_re, u_im)))
        at = slice(j * toks, (j + 1) * toks)
        for k in range(2):
            part = slice(k * toks, (k + 1) * toks)
            own_ref[part, at] = jnp.where(low, halves[0][k], halves[1][k])
            send_ref[part, at] = jnp.where(low, halves[1][k], halves[0][k])


def transform_b(own_ref, got_ref, last_ref, out_ref):
    chips, _, rows, toks = out_ref.shape
    core = lax.rem(lax.axis_index("col"), CORES)
    z = jnp.dot(last_ref[core], own_ref[...], preferred_element_type=F32)
    z += jnp.dot(last_ref[1 - core], got_ref[...], preferred_element_type=F32)
    z = z.astype(BF16)
    for j in range(CORES):
        out_ref[:, j] = z[:, j * toks : (j + 1) * toks].reshape(chips, rows, toks)


def merge_out(x_ref, merge_ref, w_ref, out_hbm, out_v, sems):
    feats = x_ref.shape[0]
    width = w_ref.shape[1]
    pieces = []
    for g in range(feats // GROUP_CH):
        at = slice(g * GROUP_CH, (g + 1) * GROUP_CH)
        pieces.append(
            lax.dot_general(
                x_ref[at, :], merge_ref[...], (((0,), (0,)), ((), ())), preferred_element_type=F32
            ).astype(BF16)
        )
    spectrum = jnp.concatenate(pieces, axis=1)
    part = width // CHUNKS
    copies = []
    for j in range(CHUNKS):
        at = slice(j * part, (j + 1) * part)
        out_v[:, at] = jnp.dot(spectrum, w_ref[:, at], preferred_element_type=F32).astype(BF16)
        copies.append(
            pltpu.make_async_copy(
                out_v.at[:, pl.ds(j * part, part)],
                out_hbm.at[0, :, pl.ds(j * part, part)],
                sems.at[j],
            )
        )
        copies[-1].start()
    for copy in copies:
        copy.wait()


VMEM = pl.BlockSpec(memory_space=pltpu.VMEM)
HBM = pl.BlockSpec(memory_space=pltpu.HBM)


def call_project(tokens, norm_gain, w_in, spread):
    _, toks, width = tokens.shape
    feats = w_in.shape[1]
    return pl.pallas_call(
        project,
        out_shape=jax.ShapeDtypeStruct((feats, toks), BF16),
        in_specs=[HBM, HBM, HBM, HBM],
        out_specs=HBM,
        scratch_shapes=[
            pltpu.VMEM((toks, width), BF16),
            pltpu.VMEM((width, feats), BF16),
            pltpu.VMEM(norm_gain.shape, BF16),
            pltpu.VMEM(spread.shape, BF16),
            pltpu.VMEM((feats, toks), BF16),
            pltpu.SemaphoreType.DMA((2, CHUNKS)),
            pltpu.SemaphoreType.DMA((2,)),
            pltpu.SemaphoreType.DMA((feats // GROUP_CH,)),
        ],
        compiler_params=pltpu.CompilerParams(vmem_limit_bytes=PROJECT_LIMIT),
        name="project",
    )(tokens, norm_gain, w_in, spread)


def call_transform_a(x, first, turn):
    toks = x.shape[-1]
    half = jax.ShapeDtypeStruct((2 * toks, CORES * toks), BF16)
    return pl.pallas_call(
        transform_a,
        out_shape=(half, half),
        in_specs=[VMEM, VMEM, VMEM],
        out_specs=(VMEM, VMEM),
        compiler_params=pltpu.CompilerParams(vmem_limit_bytes=VMEM_LIMIT),
        name="transform_a",
    )(x, first, turn)


def call_transform_b(own, got, last, shape):
    return pl.pallas_call(
        transform_b,
        out_shape=jax.ShapeDtypeStruct(shape, BF16),
        in_specs=[VMEM, VMEM, VMEM],
        out_specs=VMEM,
        compiler_params=pltpu.CompilerParams(vmem_limit_bytes=VMEM_LIMIT),
        name="transform_b",
    )(own, got, last)


def call_merge_out(x, merge, w_out):
    width = w_out.shape[1]
    toks = x.shape[1]
    return pl.pallas_call(
        merge_out,
        out_shape=jax.ShapeDtypeStruct((1, toks, width), BF16),
        in_specs=[VMEM, VMEM, VMEM],
        out_specs=HBM,
        scratch_shapes=[pltpu.VMEM((toks, width), BF16), pltpu.SemaphoreType.DMA((CHUNKS,))],
        compiler_params=pltpu.CompilerParams(vmem_limit_bytes=VMEM_LIMIT),
        name="merge_out",
    )(x, merge, w_out)


def shards(rows, cols, tokens, norm_gain, w_in, w_out):
    _, toks, width = tokens.shape
    feats = w_in.shape[1]
    chips = cols // CORES
    spread, merge = channel_tables()
    first, turn, last = sequence_tables(rows, chips, toks)
    lines = [[CORES * y + c for y in range(chips)] for c in range(CORES)]
    pairs = [(i, i ^ 1) for i in range(cols)]

    def along_row(x):
        return lax.all_to_all(x, "row", split_axis=0, concat_axis=0, tiled=True)

    def along_line(x):
        return lax.all_to_all(
            x, "col", split_axis=0, concat_axis=0, tiled=True, axis_index_groups=lines
        )

    sent = call_project(tokens, norm_gain, w_in, jnp.asarray(spread, BF16))
    sent = along_row(sent.reshape(rows, cols, toks))
    sent = along_line(sent.transpose(1, 0, 2))
    shape = (chips, CORES, rows, toks)
    own, give = call_transform_a(
        sent.reshape(shape), jnp.asarray(first, BF16), jnp.asarray(turn, F32)
    )
    got = lax.ppermute(give, "col", pairs)
    back = call_transform_b(own, got, jnp.asarray(last, BF16), shape)
    back = along_line(back.reshape(cols, rows, toks))
    back = along_row(back.transpose(1, 0, 2))
    return call_merge_out(back.reshape(feats, toks), jnp.asarray(merge, BF16), w_out)


def solution(mesh):
    return jax.shard_map(
        functools.partial(shards, mesh.shape["row"], mesh.shape["col"]),
        mesh=mesh,
        in_specs=(P("grp", ("row", "col"), None), P(), P(), P()),
        out_specs=P("grp", ("row", "col"), None),
        check_vma=False,
    )
```

```python
import functools
import math

import jax
import jax.numpy as jnp
import numpy as np
from jax import lax
from jax.experimental import pallas as pl
from jax.experimental.pallas import tpu as pltpu
from jax.sharding import PartitionSpec as P

GROUP_CH = 128
NORM_EPS = 1e-06
CORES = 2
IN_PARTS = 2
OUT_PARTS = 4
VMEM_LIMIT = 16 * 1024 * 1024
PROJECT_LIMIT = 60 * 1024 * 1024

BF16 = jnp.bfloat16
F32 = jnp.float32


def channel_tables():
    half = GROUP_CH // 2
    q = np.arange(GROUP_CH)[:, None]
    f = np.arange(GROUP_CH)[None, :]
    freq = np.where(f <= half, f, GROUP_CH - f)
    angle = 2.0 * np.pi * (q * freq % GROUP_CH) / GROUP_CH
    spread = np.where(f <= half, np.cos(angle), np.sin(angle))
    merge = np.zeros((GROUP_CH, GROUP_CH))
    merge[0, 0] = merge[half, half] = 1.0
    for m in range(1, half):
        merge[m, m] = merge[m, GROUP_CH - m] = 1.0
        merge[GROUP_CH - m, m] = -1.0
        merge[GROUP_CH - m, GROUP_CH - m] = 1.0
    return spread, merge


def sequence_tables(rows, chips, toks):
    length = rows * chips * CORES * toks
    low = CORES * toks
    high = rows * chips
    assert high == low
    a = (np.arange(rows)[None, :] * chips + np.arange(chips)[:, None]).reshape(-1)
    k1 = np.arange(high)
    b = np.arange(low)
    first = 2.0 * np.pi * (a[:, None] * k1[None, :] % high) / high
    turn = 2.0 * np.pi * (b[:, None] * k1[None, :] % length) / length
    last = 2.0 * np.pi * (a[:, None] * b[None, :] % low) / low
    scale = 1.0 / math.sqrt(length * GROUP_CH)

    def halves(table):
        return [table[..., h * toks : (h + 1) * toks] for h in range(CORES)]

    first = np.concatenate([f(t) for t in halves(first) for f in (np.cos, lambda v: -np.sin(v))], axis=1)
    turn = np.stack(
        [
            np.stack([np.stack([np.cos(t), -np.sin(t)]) * scale for t in halves(turn[c * toks : (c + 1) * toks])])
            for c in range(CORES)
        ]
    )
    last = np.stack([np.concatenate([np.cos(t), np.sin(t)], axis=1) for t in halves(last)])
    return first, turn, last


def project(tok_hbm, gain_hbm, w_hbm, spread_hbm, out_ref, tok_v, w_v, gain_v, spread_v, sems, small_sems):
    toks, width = tok_v.shape
    part = width // IN_PARTS
    small = [
        pltpu.make_async_copy(gain_hbm, gain_v, small_sems.at[0]),
        pltpu.make_async_copy(spread_hbm, spread_v, small_sems.at[1]),
    ]
    copies = []
    for j in range(IN_PARTS):
        at = pl.ds(j * part, part)
        copies.append(
            (
                pltpu.make_async_copy(tok_hbm.at[0, :, at], tok_v.at[:, at], sems.at[0, j]),
                pltpu.make_async_copy(w_hbm.at[at, :], w_v.at[at, :], sems.at[1, j]),
            )
        )
    small[0].start()
    for pair in copies:
        for copy in pair:
            copy.start()
    small[1].start()
    small[0].wait()
    gain = gain_v[...].astype(F32).reshape(1, width)
    squares = jnp.zeros((toks, 1), F32)
    total = jnp.zeros((toks, w_v.shape[1]), F32)
    for j in range(IN_PARTS):
        at = slice(j * part, (j + 1) * part)
        copies[j][0].wait()
        x = tok_v[:, at].astype(F32)
        squares += jnp.sum(x * x, axis=-1, keepdims=True)
        scaled = (x * gain[:, at]).astype(BF16)
        copies[j][1].wait()
        total += jnp.dot(scaled, w_v[at, :], preferred_element_type=F32)
    factor = lax.rsqrt(squares * (1.0 / width) + NORM_EPS)
    mixin = (total * factor).astype(BF16)
    small[1].wait()
    for g in range(w_v.shape[1] // GROUP_CH):
        at = slice(g * GROUP_CH, (g + 1) * GROUP_CH)
        out_ref[at, :] = lax.dot_general(
            spread_v[...], mixin[:, at], (((0,), (1,)), ((), ())), preferred_element_type=F32
        ).astype(BF16)


def transform_a(x_ref, first_ref, turn_ref, own_ref, send_ref):
    chips, _, rows, toks = x_ref.shape
    cols = chips * CORES
    col = lax.axis_index("col")
    core = lax.rem(col, CORES)
    feature = lax.axis_index("row") * cols + (col - core)
    low = core == 0
    for j in range(CORES):
        sine = lax.rem(feature + j, GROUP_CH) > GROUP_CH // 2
        y = lax.dot_general(
            x_ref[:, j].reshape(chips * rows, toks),
            first_ref[...],
            (((0,), (0,)), ((), ())),
            preferred_element_type=F32,
        )
        halves = []
        for h in range(CORES):
            y_re = y[:, 2 * h * toks : (2 * h + 1) * toks]
            y_im = y[:, (2 * h + 1) * toks : (2 * h + 2) * toks]
            w_re, w_im = turn_ref[core, h, 0], turn_ref[core, h, 1]
            u_re = (y_re * w_re - y_im * w_im).astype(BF16)
            u_im = (y_re * w_im + y_im * w_re).astype(BF16)
            halves.append((jnp.where(sine, -u_im, u_re), jnp.where(sine, u_re, u_im)))
        at = slice(j * toks, (j + 1) * toks)
        for k in range(2):
            part = slice(k * toks, (k + 1) * toks)
            own_ref[part, at] = jnp.where(low, halves[0][k], halves[1][k])
            send_ref[part, at] = jnp.where(low, halves[1][k], halves[0][k])


def transform_b(own_ref, got_ref, last_ref, out_ref):
    chips, _, rows, toks = out_ref.shape
    core = lax.rem(lax.axis_index("col"), CORES)
    z = jnp.dot(last_ref[core], own_ref[...], preferred_element_type=F32)
    z += jnp.dot(last_ref[1 - core], got_ref[...], preferred_element_type=F32)
    z = z.astype(BF16)
    for j in range(CORES):
        out_ref[:, j] = z[:, j * toks : (j + 1) * toks].reshape(chips, rows, toks)


def merge_out(x_ref, merge_ref, w_ref, out_hbm, out_v, sems):
    feats = x_ref.shape[0]
    width = w_ref.shape[1]
    pieces = []
    for g in range(feats // GROUP_CH):
        at = slice(g * GROUP_CH, (g + 1) * GROUP_CH)
        pieces.append(
            lax.dot_general(
                x_ref[at, :], merge_ref[...], (((0,), (0,)), ((), ())), preferred_element_type=F32
            ).astype(BF16)
        )
    spectrum = jnp.concatenate(pieces, axis=1)
    part = width // OUT_PARTS
    copies = []
    for j in range(OUT_PARTS):
        at = slice(j * part, (j + 1) * part)
        out_v[:, at] = jnp.dot(spectrum, w_ref[:, at], preferred_element_type=F32).astype(BF16)
        copies.append(
            pltpu.make_async_copy(
                out_v.at[:, pl.ds(j * part, part)],
                out_hbm.at[0, :, pl.ds(j * part, part)],
                sems.at[j],
            )
        )
        copies[-1].start()
    for copy in copies:
        copy.wait()


VMEM = pl.BlockSpec(memory_space=pltpu.VMEM)
HBM = pl.BlockSpec(memory_space=pltpu.HBM)


def call_project(tokens, norm_gain, w_in, spread):
    _, toks, width = tokens.shape
    feats = w_in.shape[1]
    return pl.pallas_call(
        project,
        out_shape=pltpu.VMEM((feats, toks), BF16),
        in_specs=[HBM, HBM, HBM, HBM],
        out_specs=VMEM,
        scratch_shapes=[
            pltpu.VMEM((toks, width), BF16),
            pltpu.VMEM((width, feats), BF16),
            pltpu.VMEM(norm_gain.shape, BF16),
            pltpu.VMEM(spread.shape, BF16),
            pltpu.SemaphoreType.DMA((2, IN_PARTS)),
            pltpu.SemaphoreType.DMA((2,)),
        ],
        compiler_params=pltpu.CompilerParams(vmem_limit_bytes=PROJECT_LIMIT),
        name="project",
    )(tokens, norm_gain, w_in, spread)


def call_transform_a(x, first, turn):
    toks = x.shape[-1]
    half = jax.ShapeDtypeStruct((2 * toks, CORES * toks), BF16)
    return pl.pallas_call(
        transform_a,
        out_shape=(half, half),
        in_specs=[VMEM, VMEM, VMEM],
        out_specs=(VMEM, VMEM),
        compiler_params=pltpu.CompilerParams(vmem_limit_bytes=VMEM_LIMIT),
        name="transform_a",
    )(x, first, turn)


def call_transform_b(own, got, last, shape):
    return pl.pallas_call(
        transform_b,
        out_shape=jax.ShapeDtypeStruct(shape, BF16),
        in_specs=[VMEM, VMEM, VMEM],
        out_specs=VMEM,
        compiler_params=pltpu.CompilerParams(vmem_limit_bytes=VMEM_LIMIT),
        name="transform_b",
    )(own, got, last)


def call_merge_out(x, merge, w_out):
    width = w_out.shape[1]
    toks = x.shape[1]
    return pl.pallas_call(
        merge_out,
        out_shape=jax.ShapeDtypeStruct((1, toks, width), BF16),
        in_specs=[VMEM, VMEM, VMEM],
        out_specs=HBM,
        scratch_shapes=[pltpu.VMEM((toks, width), BF16), pltpu.SemaphoreType.DMA((OUT_PARTS,))],
        compiler_params=pltpu.CompilerParams(vmem_limit_bytes=VMEM_LIMIT),
        name="merge_out",
    )(x, merge, w_out)


def shards(rows, cols, tokens, norm_gain, w_in, w_out):
    _, toks, width = tokens.shape
    feats = w_in.shape[1]
    chips = cols // CORES
    spread, merge = channel_tables()
    first, turn, last = sequence_tables(rows, chips, toks)
    lines = [[CORES * y + c for y in range(chips)] for c in range(CORES)]
    pairs = [(i, i ^ 1) for i in range(cols)]

    def along_row(x):
        return lax.all_to_all(x, "row", split_axis=0, concat_axis=0, tiled=True)

    def along_line(x):
        return lax.all_to_all(
            x, "col", split_axis=0, concat_axis=0, tiled=True, axis_index_groups=lines
        )

    sent = call_project(tokens, norm_gain, w_in, jnp.asarray(spread, BF16))
    sent = along_row(sent.reshape(rows, cols, toks))
    sent = along_line(sent.transpose(1, 0, 2))
    shape = (chips, CORES, rows, toks)
    own, give = call_transform_a(
        sent.reshape(shape), jnp.asarray(first, BF16), jnp.asarray(turn, F32)
    )
    got = lax.ppermute(give, "col", pairs)
    back = call_transform_b(own, got, jnp.asarray(last, BF16), shape)
    back = along_line(back.reshape(cols, rows, toks))
    back = along_row(back.transpose(1, 0, 2))
    return call_merge_out(back.reshape(feats, toks), jnp.asarray(merge, BF16), w_out)


def solution(mesh):
    return jax.shard_map(
        functools.partial(shards, mesh.shape["row"], mesh.shape["col"]),
        mesh=mesh,
        in_specs=(P("grp", ("row", "col"), None), P(), P(), P()),
        out_specs=P("grp", ("row", "col"), None),
        check_vma=False,
    )
```

```python
import functools
import math

import jax
import jax.numpy as jnp
import numpy as np
from jax import lax
from jax.experimental import pallas as pl
from jax.experimental.pallas import tpu as pltpu
from jax.sharding import PartitionSpec as P

GROUP_CH = 128
NORM_EPS = 1e-06
CORES = 2
IN_PARTS = 2
OUT_PARTS = 4
VMEM_LIMIT = 16 * 1024 * 1024
PROJECT_LIMIT = 60 * 1024 * 1024

BF16 = jnp.bfloat16
F32 = jnp.float32


def channel_tables():
    half = GROUP_CH // 2
    q = np.arange(GROUP_CH)[:, None]
    f = np.arange(GROUP_CH)[None, :]
    freq = np.where(f <= half, f, GROUP_CH - f)
    angle = 2.0 * np.pi * (q * freq % GROUP_CH) / GROUP_CH
    spread = np.where(f <= half, np.cos(angle), np.sin(angle))
    merge = np.zeros((GROUP_CH, GROUP_CH))
    merge[0, 0] = merge[half, half] = 1.0
    for m in range(1, half):
        merge[m, m] = merge[m, GROUP_CH - m] = 1.0
        merge[GROUP_CH - m, m] = -1.0
        merge[GROUP_CH - m, GROUP_CH - m] = 1.0
    return spread, merge


def sequence_tables(rows, chips, toks):
    length = rows * chips * CORES * toks
    low = CORES * toks
    high = rows * chips
    assert high == low
    a = np.arange(high)
    b = np.arange(low)
    first = 2.0 * np.pi * (a[:, None] * a[None, :] % high) / high
    turn = 2.0 * np.pi * (b[:, None] * a[None, :] % length) / length
    last = 2.0 * np.pi * (a[:, None] * b[None, :] % low) / low
    scale = 1.0 / math.sqrt(length * GROUP_CH)
    spread = np.zeros((high, CORES, 2, toks))
    gather = np.zeros((CORES, high, 2, toks))
    turns = np.zeros((CORES, CORES, 2, toks, toks))
    for h in range(CORES):
        at = slice(h * toks, (h + 1) * toks)
        spread[:, h, 0] = np.cos(first[:, at])
        spread[:, h, 1] = -np.sin(first[:, at])
        gather[h, :, 0] = np.cos(last[:, at])
        gather[h, :, 1] = np.sin(last[:, at])
        for c in range(CORES):
            angle = turn[c * toks : (c + 1) * toks, at]
            turns[c, h, 0] = np.cos(angle) * scale
            turns[c, h, 1] = -np.sin(angle) * scale
    return spread.reshape(high, -1), turns, gather.reshape(CORES, high, -1)


def project(tok_hbm, gain_hbm, w_hbm, spread_hbm, out_ref, tok_v, w_v, gain_v, spread_v, sems, small_sems):
    toks, width = tok_v.shape
    part = width // IN_PARTS
    small = [
        pltpu.make_async_copy(gain_hbm, gain_v, small_sems.at[0]),
        pltpu.make_async_copy(spread_hbm, spread_v, small_sems.at[1]),
    ]
    copies = []
    for j in range(IN_PARTS):
        at = pl.ds(j * part, part)
        copies.append(
            (
                pltpu.make_async_copy(tok_hbm.at[0, :, at], tok_v.at[:, at], sems.at[0, j]),
                pltpu.make_async_copy(w_hbm.at[at, :], w_v.at[at, :], sems.at[1, j]),
            )
        )
    small[0].start()
    for pair in copies:
        for copy in pair:
            copy.start()
    small[1].start()
    small[0].wait()
    gain = gain_v[...].astype(F32).reshape(1, width)
    squares = jnp.zeros((toks, 1), F32)
    total = jnp.zeros((toks, w_v.shape[1]), F32)
    for j in range(IN_PARTS):
        at = slice(j * part, (j + 1) * part)
        copies[j][0].wait()
        x = tok_v[:, at].astype(F32)
        squares += jnp.sum(x * x, axis=-1, keepdims=True)
        scaled = (x * gain[:, at]).astype(BF16)
        copies[j][1].wait()
        total += jnp.dot(scaled, w_v[at, :], preferred_element_type=F32)
    factor = lax.rsqrt(squares * (1.0 / width) + NORM_EPS)
    mixin = (total * factor).astype(BF16)
    small[1].wait()
    for g in range(w_v.shape[1] // GROUP_CH):
        at = slice(g * GROUP_CH, (g + 1) * GROUP_CH)
        out_ref[at, :] = lax.dot_general(
            spread_v[...], mixin[:, at], (((0,), (1,)), ((), ())), preferred_element_type=F32
        ).astype(BF16)


def transform_a(x_ref, first_ref, turn_ref, own_ref, send_ref, wide):
    count, toks = x_ref.shape
    wide[...] = x_ref[...].astype(F32)
    core = lax.axis_index("core")
    feature = (lax.axis_index("row") * lax.axis_size("y") + lax.axis_index("y")) * CORES
    low = core == 0
    for j in range(CORES):
        x = wide[pl.ds(j, count // CORES, stride=CORES), :].astype(BF16)
        y = lax.dot_general(
            x, first_ref[...], (((0,), (0,)), ((), ())), preferred_element_type=F32
        )
        sine = lax.rem(feature + j, GROUP_CH) > GROUP_CH // 2
        halves = []
        for h in range(CORES):
            at = 2 * h * toks
            y_re, y_im = y[:, at : at + toks], y[:, at + toks : at + 2 * toks]
            w_re, w_im = turn_ref[core, h, 0], turn_ref[core, h, 1]
            u_re = (y_re * w_re - y_im * w_im).astype(BF16)
            u_im = (y_re * w_im + y_im * w_re).astype(BF16)
            halves.append((jnp.where(sine, -u_im, u_re), jnp.where(sine, u_re, u_im)))
        for k in range(2):
            part = slice((2 * j + k) * toks, (2 * j + k + 1) * toks)
            own_ref[part, :] = jnp.where(low, halves[0][k], halves[1][k])
            send_ref[part, :] = jnp.where(low, halves[1][k], halves[0][k])


def transform_b(own_ref, got_ref, last_ref, out_ref, wide):
    core = lax.axis_index("core")
    count = wide.shape[0] // CORES
    part = own_ref.shape[0] // CORES
    for j in range(CORES):
        at = slice(j * part, (j + 1) * part)
        z = jnp.dot(last_ref[core], own_ref[at, :], preferred_element_type=F32)
        z += jnp.dot(last_ref[1 - core], got_ref[at, :], preferred_element_type=F32)
        wide[pl.ds(j, count, stride=CORES), :] = z
    out_ref[...] = wide[...].astype(BF16)


def merge_out(x_ref, merge_ref, w_ref, out_hbm, out_v, sems):
    feats = x_ref.shape[0]
    width = w_ref.shape[1]
    pieces = []
    for g in range(feats // GROUP_CH):
        at = slice(g * GROUP_CH, (g + 1) * GROUP_CH)
        pieces.append(
            lax.dot_general(
                x_ref[at, :], merge_ref[...], (((0,), (0,)), ((), ())), preferred_element_type=F32
            ).astype(BF16)
        )
    spectrum = jnp.concatenate(pieces, axis=1)
    part = width // OUT_PARTS
    copies = []
    for j in range(OUT_PARTS):
        at = slice(j * part, (j + 1) * part)
        out_v[:, at] = jnp.dot(spectrum, w_ref[:, at], preferred_element_type=F32).astype(BF16)
        copies.append(
            pltpu.make_async_copy(
                out_v.at[:, pl.ds(j * part, part)],
                out_hbm.at[0, :, pl.ds(j * part, part)],
                sems.at[j],
            )
        )
        copies[-1].start()
    for copy in copies:
        copy.wait()


VMEM = pl.BlockSpec(memory_space=pltpu.VMEM)
HBM = pl.BlockSpec(memory_space=pltpu.HBM)


def call_project(tokens, norm_gain, w_in, spread):
    _, toks, width = tokens.shape
    feats = w_in.shape[1]
    return pl.pallas_call(
        project,
        out_shape=pltpu.VMEM((feats, toks), BF16),
        in_specs=[HBM, HBM, HBM, HBM],
        out_specs=VMEM,
        scratch_shapes=[
            pltpu.VMEM((toks, width), BF16),
            pltpu.VMEM((width, feats), BF16),
            pltpu.VMEM(norm_gain.shape, BF16),
            pltpu.VMEM(spread.shape, BF16),
            pltpu.SemaphoreType.DMA((2, IN_PARTS)),
            pltpu.SemaphoreType.DMA((2,)),
        ],
        compiler_params=pltpu.CompilerParams(vmem_limit_bytes=PROJECT_LIMIT),
        name="project",
    )(tokens, norm_gain, w_in, spread)


def call_transform_a(x, first, turn):
    half = jax.ShapeDtypeStruct((2 * CORES * x.shape[1], x.shape[1]), BF16)
    return pl.pallas_call(
        transform_a,
        out_shape=(half, half),
        in_specs=[VMEM, VMEM, VMEM],
        out_specs=(VMEM, VMEM),
        scratch_shapes=[pltpu.VMEM(x.shape, F32)],
        compiler_params=pltpu.CompilerParams(vmem_limit_bytes=VMEM_LIMIT),
        name="transform_a",
    )(x, first, turn)


def call_transform_b(own, got, last):
    shape = (CORES * last.shape[1], own.shape[1])
    return pl.pallas_call(
        transform_b,
        out_shape=jax.ShapeDtypeStruct(shape, BF16),
        in_specs=[VMEM, VMEM, VMEM],
        out_specs=VMEM,
        scratch_shapes=[pltpu.VMEM(shape, F32)],
        compiler_params=pltpu.CompilerParams(vmem_limit_bytes=VMEM_LIMIT),
        name="transform_b",
    )(own, got, last)


def call_merge_out(x, merge, w_out):
    width = w_out.shape[1]
    toks = x.shape[1]
    return pl.pallas_call(
        merge_out,
        out_shape=jax.ShapeDtypeStruct((1, toks, width), BF16),
        in_specs=[VMEM, VMEM, VMEM],
        out_specs=HBM,
        scratch_shapes=[pltpu.VMEM((toks, width), BF16), pltpu.SemaphoreType.DMA((OUT_PARTS,))],
        compiler_params=pltpu.CompilerParams(vmem_limit_bytes=VMEM_LIMIT),
        name="merge_out",
    )(x, merge, w_out)


def shards(rows, chips, tokens, norm_gain, w_in, w_out):
    _, toks, width = tokens.shape
    feats = w_in.shape[1]
    spread, merge = channel_tables()
    first, turn, last = sequence_tables(rows, chips, toks)

    def exchange(x):
        x = x.reshape(rows * chips, CORES, toks)
        x = lax.all_to_all(x, ("row", "y"), split_axis=0, concat_axis=0, tiled=True)
        return x.reshape(feats, toks)

    sent = exchange(call_project(tokens, norm_gain, w_in, jnp.asarray(spread, BF16)))
    own, give = call_transform_a(sent, jnp.asarray(first, BF16), jnp.asarray(turn, F32))
    got = lax.ppermute(give, "core", [(0, 1), (1, 0)])
    back = exchange(call_transform_b(own, got, jnp.asarray(last, BF16)))
    return call_merge_out(back, jnp.asarray(merge, BF16), w_out)


def solution(mesh):
    groups, rows, cols = (mesh.shape[name] for name in ("grp", "row", "col"))
    chips = cols // CORES
    split = jax.sharding.Mesh(
        mesh.devices.reshape(groups, rows, chips, CORES), ("grp", "row", "y", "core")
    )
    spec = P("grp", ("row", "y", "core"), None)
    return jax.shard_map(
        functools.partial(shards, rows, chips),
        mesh=split,
        in_specs=(spec, P(), P(), P()),
        out_specs=spec,
        check_vma=False,
    )
```

```python
import functools
import math

import jax
import jax.numpy as jnp
import numpy as np
from jax import lax
from jax.experimental import pallas as pl
from jax.experimental.pallas import tpu as pltpu
from jax.sharding import PartitionSpec as P

GROUP_CH = 128
NORM_EPS = 1e-06
CORES = 2
IN_PARTS = 2
OUT_PARTS = 4
VMEM_LIMIT = 16 * 1024 * 1024
PROJECT_LIMIT = 60 * 1024 * 1024

BF16 = jnp.bfloat16
F32 = jnp.float32


def channel_tables():
    half = GROUP_CH // 2
    q = np.arange(GROUP_CH)[:, None]
    f = np.arange(GROUP_CH)[None, :]
    freq = np.where(f <= half, f, GROUP_CH - f)
    angle = 2.0 * np.pi * (q * freq % GROUP_CH) / GROUP_CH
    spread = np.where(f <= half, np.cos(angle), np.sin(angle))
    merge = np.zeros((GROUP_CH, GROUP_CH))
    merge[0, 0] = merge[half, half] = 1.0
    for m in range(1, half):
        merge[m, m] = merge[m, GROUP_CH - m] = 1.0
        merge[GROUP_CH - m, m] = -1.0
        merge[GROUP_CH - m, GROUP_CH - m] = 1.0
    return spread, merge


def sequence_tables(rows, chips, toks):
    length = rows * chips * CORES * toks
    low = CORES * toks
    high = rows * chips
    assert high == low
    a = np.arange(high)
    b = np.arange(low)
    first = 2.0 * np.pi * (a[:, None] * a[None, :] % high) / high
    turn = 2.0 * np.pi * (b[:, None] * a[None, :] % length) / length
    last = 2.0 * np.pi * (a[:, None] * b[None, :] % low) / low
    scale = 1.0 / math.sqrt(length * GROUP_CH)
    spread = np.zeros((high, CORES, 2, toks))
    gather = np.zeros((CORES, high, 2, toks))
    turns = np.zeros((CORES, CORES, 2, toks, toks))
    for h in range(CORES):
        at = slice(h * toks, (h + 1) * toks)
        spread[:, h, 0] = np.cos(first[:, at])
        spread[:, h, 1] = -np.sin(first[:, at])
        gather[h, :, 0] = np.cos(last[:, at])
        gather[h, :, 1] = np.sin(last[:, at])
        for c in range(CORES):
            angle = turn[c * toks : (c + 1) * toks, at]
            turns[c, h, 0] = np.cos(angle) * scale
            turns[c, h, 1] = -np.sin(angle) * scale
    return spread.reshape(high, -1), turns, gather.reshape(CORES, high, -1)


def project(tok_hbm, gain_hbm, w_hbm, spread_hbm, out_ref, tok_v, w_v, gain_v, spread_v, sems, small_sems):
    toks, width = tok_v.shape
    part = width // IN_PARTS
    small = [
        pltpu.make_async_copy(gain_hbm, gain_v, small_sems.at[0]),
        pltpu.make_async_copy(spread_hbm, spread_v, small_sems.at[1]),
    ]
    copies = []
    for j in range(IN_PARTS):
        at = pl.ds(j * part, part)
        copies.append(
            (
                pltpu.make_async_copy(tok_hbm.at[0, :, at], tok_v.at[:, at], sems.at[0, j]),
                pltpu.make_async_copy(w_hbm.at[at, :], w_v.at[at, :], sems.at[1, j]),
            )
        )
    small[0].start()
    for pair in copies:
        for copy in pair:
            copy.start()
    small[1].start()
    small[0].wait()
    gain = gain_v[...].astype(F32).reshape(1, width)
    squares = jnp.zeros((toks, 1), F32)
    total = jnp.zeros((toks, w_v.shape[1]), F32)
    for j in range(IN_PARTS):
        at = slice(j * part, (j + 1) * part)
        copies[j][0].wait()
        x = tok_v[:, at].astype(F32)
        squares += jnp.sum(x * x, axis=-1, keepdims=True)
        scaled = (x * gain[:, at]).astype(BF16)
        copies[j][1].wait()
        total += jnp.dot(scaled, w_v[at, :], preferred_element_type=F32)
    factor = lax.rsqrt(squares * (1.0 / width) + NORM_EPS)
    mixin = (total * factor).astype(BF16)
    small[1].wait()
    for g in range(w_v.shape[1] // GROUP_CH):
        at = slice(g * GROUP_CH, (g + 1) * GROUP_CH)
        out_ref[at, :] = lax.dot_general(
            spread_v[...], mixin[:, at], (((0,), (1,)), ((), ())), preferred_element_type=F32
        ).astype(BF16)


def transform_a(x_ref, first_ref, turn_ref, own_ref, send_ref, wide):
    count, toks = x_ref.shape
    wide[...] = x_ref[...].astype(F32)
    core = lax.axis_index("core")
    feature = (lax.axis_index("row") * lax.axis_size("y") + lax.axis_index("y")) * CORES
    low = core == 0
    for j in range(CORES):
        x = wide[pl.ds(j, count // CORES, stride=CORES), :].astype(BF16)
        y = lax.dot_general(
            x, first_ref[...], (((0,), (0,)), ((), ())), preferred_element_type=F32
        )
        sine = lax.rem(feature + j, GROUP_CH) > GROUP_CH // 2
        halves = []
        for h in range(CORES):
            at = 2 * h * toks
            y_re, y_im = y[:, at : at + toks], y[:, at + toks : at + 2 * toks]
            w_re, w_im = turn_ref[core, h, 0], turn_ref[core, h, 1]
            u_re = (y_re * w_re - y_im * w_im).astype(BF16)
            u_im = (y_re * w_im + y_im * w_re).astype(BF16)
            halves.append((jnp.where(sine, -u_im, u_re), jnp.where(sine, u_re, u_im)))
        for k in range(2):
            part = slice((2 * j + k) * toks, (2 * j + k + 1) * toks)
            own_ref[part, :] = jnp.where(low, halves[0][k], halves[1][k])
            send_ref[part, :] = jnp.where(low, halves[1][k], halves[0][k])


def transform_b(own_ref, got_ref, last_ref, out_ref, wide):
    core = lax.axis_index("core")
    count = wide.shape[0] // CORES
    part = own_ref.shape[0] // CORES
    for j in range(CORES):
        at = slice(j * part, (j + 1) * part)
        z = jnp.dot(last_ref[core], own_ref[at, :], preferred_element_type=F32)
        z += jnp.dot(last_ref[1 - core], got_ref[1 - core, at, :], preferred_element_type=F32)
        wide[pl.ds(j, count, stride=CORES), :] = z
    out_ref[...] = wide[...].astype(BF16)


def merge_out(x_ref, merge_ref, w_ref, out_hbm, out_v, sems):
    feats = x_ref.shape[0]
    width = w_ref.shape[1]
    pieces = []
    for g in range(feats // GROUP_CH):
        at = slice(g * GROUP_CH, (g + 1) * GROUP_CH)
        pieces.append(
            lax.dot_general(
                x_ref[at, :], merge_ref[...], (((0,), (0,)), ((), ())), preferred_element_type=F32
            ).astype(BF16)
        )
    spectrum = jnp.concatenate(pieces, axis=1)
    part = width // OUT_PARTS
    copies = []
    for j in range(OUT_PARTS):
        at = slice(j * part, (j + 1) * part)
        out_v[:, at] = jnp.dot(spectrum, w_ref[:, at], preferred_element_type=F32).astype(BF16)
        copies.append(
            pltpu.make_async_copy(
                out_v.at[:, pl.ds(j * part, part)],
                out_hbm.at[0, :, pl.ds(j * part, part)],
                sems.at[j],
            )
        )
        copies[-1].start()
    for copy in copies:
        copy.wait()


VMEM = pl.BlockSpec(memory_space=pltpu.VMEM)
HBM = pl.BlockSpec(memory_space=pltpu.HBM)


def call_project(tokens, norm_gain, w_in, spread):
    _, toks, width = tokens.shape
    feats = w_in.shape[1]
    return pl.pallas_call(
        project,
        out_shape=pltpu.VMEM((feats, toks), BF16),
        in_specs=[HBM, HBM, HBM, HBM],
        out_specs=VMEM,
        scratch_shapes=[
            pltpu.VMEM((toks, width), BF16),
            pltpu.VMEM((width, feats), BF16),
            pltpu.VMEM(norm_gain.shape, BF16),
            pltpu.VMEM(spread.shape, BF16),
            pltpu.SemaphoreType.DMA((2, IN_PARTS)),
            pltpu.SemaphoreType.DMA((2,)),
        ],
        compiler_params=pltpu.CompilerParams(vmem_limit_bytes=PROJECT_LIMIT),
        name="project",
    )(tokens, norm_gain, w_in, spread)


def call_transform_a(x, first, turn):
    half = jax.ShapeDtypeStruct((2 * CORES * x.shape[1], x.shape[1]), BF16)
    return pl.pallas_call(
        transform_a,
        out_shape=(half, half),
        in_specs=[VMEM, VMEM, VMEM],
        out_specs=(VMEM, VMEM),
        scratch_shapes=[pltpu.VMEM(x.shape, F32)],
        compiler_params=pltpu.CompilerParams(vmem_limit_bytes=VMEM_LIMIT),
        name="transform_a",
    )(x, first, turn)


def call_transform_b(own, got, last):
    shape = (CORES * last.shape[1], own.shape[1])
    return pl.pallas_call(
        transform_b,
        out_shape=jax.ShapeDtypeStruct(shape, BF16),
        in_specs=[VMEM, VMEM, VMEM],
        out_specs=VMEM,
        scratch_shapes=[pltpu.VMEM(shape, F32)],
        compiler_params=pltpu.CompilerParams(vmem_limit_bytes=VMEM_LIMIT),
        name="transform_b",
    )(own, got, last)


def call_merge_out(x, merge, w_out):
    width = w_out.shape[1]
    toks = x.shape[1]
    return pl.pallas_call(
        merge_out,
        out_shape=jax.ShapeDtypeStruct((1, toks, width), BF16),
        in_specs=[VMEM, VMEM, VMEM],
        out_specs=HBM,
        scratch_shapes=[pltpu.VMEM((toks, width), BF16), pltpu.SemaphoreType.DMA((OUT_PARTS,))],
        compiler_params=pltpu.CompilerParams(vmem_limit_bytes=VMEM_LIMIT),
        name="merge_out",
    )(x, merge, w_out)


def shards(rows, chips, tokens, norm_gain, w_in, w_out):
    _, toks, width = tokens.shape
    feats = w_in.shape[1]
    spread, merge = channel_tables()
    first, turn, last = sequence_tables(rows, chips, toks)

    def exchange(x):
        x = x.reshape(rows * chips, CORES, toks)
        x = lax.all_to_all(x, ("row", "y"), split_axis=0, concat_axis=0, tiled=True)
        return x.reshape(feats, toks)

    sent = exchange(call_project(tokens, norm_gain, w_in, jnp.asarray(spread, BF16)))
    own, give = call_transform_a(sent, jnp.asarray(first, BF16), jnp.asarray(turn, F32))
    got = lax.all_gather(give, "core")
    back = exchange(call_transform_b(own, got, jnp.asarray(last, BF16)))
    return call_merge_out(back, jnp.asarray(merge, BF16), w_out)


def solution(mesh):
    groups, rows, cols = (mesh.shape[name] for name in ("grp", "row", "col"))
    chips = cols // CORES
    split = jax.sharding.Mesh(
        mesh.devices.reshape(groups, rows, chips, CORES), ("grp", "row", "y", "core")
    )
    spec = P("grp", ("row", "y", "core"), None)
    return jax.shard_map(
        functools.partial(shards, rows, chips),
        mesh=split,
        in_specs=(spec, P(), P(), P()),
        out_specs=spec,
        check_vma=False,
    )
```

```python
import functools
import math

import jax
import jax.numpy as jnp
import numpy as np
from jax import lax
from jax.experimental import pallas as pl
from jax.experimental.pallas import tpu as pltpu
from jax.sharding import PartitionSpec as P

GROUP_CH = 128
NORM_EPS = 1e-06
CORES = 2
IN_PARTS = 4
OUT_PARTS = 4
VMEM_LIMIT = 16 * 1024 * 1024
PROJECT_LIMIT = 60 * 1024 * 1024

BF16 = jnp.bfloat16
F32 = jnp.float32


def channel_tables():
    half = GROUP_CH // 2
    q = np.arange(GROUP_CH)[:, None]
    f = np.arange(GROUP_CH)[None, :]
    freq = np.where(f <= half, f, GROUP_CH - f)
    angle = 2.0 * np.pi * (q * freq % GROUP_CH) / GROUP_CH
    spread = np.where(f <= half, np.cos(angle), np.sin(angle))
    merge = np.zeros((GROUP_CH, GROUP_CH))
    merge[0, 0] = merge[half, half] = 1.0
    for m in range(1, half):
        merge[m, m] = merge[m, GROUP_CH - m] = 1.0
        merge[GROUP_CH - m, m] = -1.0
        merge[GROUP_CH - m, GROUP_CH - m] = 1.0
    return spread, merge


def sequence_tables(rows, chips, toks):
    length = rows * chips * CORES * toks
    low = CORES * toks
    high = rows * chips
    assert high == low
    a = np.arange(high)
    b = np.arange(low)
    first = 2.0 * np.pi * (a[:, None] * a[None, :] % high) / high
    turn = 2.0 * np.pi * (b[:, None] * a[None, :] % length) / length
    last = 2.0 * np.pi * (a[:, None] * b[None, :] % low) / low
    scale = 1.0 / math.sqrt(length * GROUP_CH)
    spread = np.zeros((high, CORES, 2, toks))
    gather = np.zeros((CORES, high, 2, toks))
    turns = np.zeros((CORES, CORES, 2, toks, toks))
    for h in range(CORES):
        at = slice(h * toks, (h + 1) * toks)
        spread[:, h, 0] = np.cos(first[:, at])
        spread[:, h, 1] = -np.sin(first[:, at])
        gather[h, :, 0] = np.cos(last[:, at])
        gather[h, :, 1] = np.sin(last[:, at])
        for c in range(CORES):
            angle = turn[c * toks : (c + 1) * toks, at]
            turns[c, h, 0] = np.cos(angle) * scale
            turns[c, h, 1] = -np.sin(angle) * scale
    return spread.reshape(high, -1), turns, gather.reshape(CORES, high, -1)


def project(
    tok_hbm, gain_hbm, w_hbm, spread_hbm, out_ref, tok_v, w_v, gain_v, spread_v, w_sems, sems
):
    toks, width = tok_v.shape
    part = width // IN_PARTS
    tok_copy = pltpu.make_async_copy(tok_hbm.at[0], tok_v, sems.at[0])
    gain_copy = pltpu.make_async_copy(gain_hbm, gain_v, sems.at[1])
    spread_copy = pltpu.make_async_copy(spread_hbm, spread_v, sems.at[2])
    w_copies = []
    for j in range(IN_PARTS):
        at = pl.ds(j * part, part)
        w_copies.append(pltpu.make_async_copy(w_hbm.at[at, :], w_v.at[at, :], w_sems.at[j]))
    for copy in [tok_copy, gain_copy, *w_copies, spread_copy]:
        copy.start()
    tok_copy.wait()
    gain_copy.wait()
    x = tok_v[...].astype(F32)
    gain = gain_v[...].astype(F32).reshape(1, width)
    factor = lax.rsqrt(jnp.mean(x * x, axis=-1, keepdims=True) + NORM_EPS)
    tok_v[...] = (x * gain).astype(BF16)
    total = jnp.zeros((toks, w_v.shape[1]), F32)
    for j in range(IN_PARTS):
        at = slice(j * part, (j + 1) * part)
        w_copies[j].wait()
        total += jnp.dot(tok_v[:, at], w_v[at, :], preferred_element_type=F32)
    mixin = (total * factor).astype(BF16)
    spread_copy.wait()
    for g in range(w_v.shape[1] // GROUP_CH):
        at = slice(g * GROUP_CH, (g + 1) * GROUP_CH)
        out_ref[at, :] = lax.dot_general(
            spread_v[...], mixin[:, at], (((0,), (1,)), ((), ())), preferred_element_type=F32
        ).astype(BF16)


def transform_a(x_ref, first_ref, turn_ref, own_ref, send_ref, wide):
    count, toks = x_ref.shape
    wide[...] = x_ref[...].astype(F32)
    core = lax.axis_index("core")
    feature = (lax.axis_index("row") * lax.axis_size("y") + lax.axis_index("y")) * CORES
    low = core == 0
    for j in range(CORES):
        x = wide[pl.ds(j, count // CORES, stride=CORES), :].astype(BF16)
        y = lax.dot_general(
            x, first_ref[...], (((0,), (0,)), ((), ())), preferred_element_type=F32
        )
        sine = lax.rem(feature + j, GROUP_CH) > GROUP_CH // 2
        halves = []
        for h in range(CORES):
            at = 2 * h * toks
            y_re, y_im = y[:, at : at + toks], y[:, at + toks : at + 2 * toks]
            w_re, w_im = turn_ref[core, h, 0], turn_ref[core, h, 1]
            u_re = (y_re * w_re - y_im * w_im).astype(BF16)
            u_im = (y_re * w_im + y_im * w_re).astype(BF16)
            halves.append((jnp.where(sine, -u_im, u_re), jnp.where(sine, u_re, u_im)))
        for k in range(2):
            part = slice((2 * j + k) * toks, (2 * j + k + 1) * toks)
            own_ref[part, :] = jnp.where(low, halves[0][k], halves[1][k])
            send_ref[part, :] = jnp.where(low, halves[1][k], halves[0][k])


def transform_b(own_ref, got_ref, last_ref, out_ref, wide):
    core = lax.axis_index("core")
    count = wide.shape[0] // CORES
    part = own_ref.shape[0] // CORES
    for j in range(CORES):
        at = slice(j * part, (j + 1) * part)
        z = jnp.dot(last_ref[core], own_ref[at, :], preferred_element_type=F32)
        z += jnp.dot(last_ref[1 - core], got_ref[1 - core, at, :], preferred_element_type=F32)
        wide[pl.ds(j, count, stride=CORES), :] = z
    out_ref[...] = wide[...].astype(BF16)


def merge_out(x_ref, merge_ref, w_ref, out_hbm, out_v, sems):
    feats = x_ref.shape[0]
    width = w_ref.shape[1]
    pieces = []
    for g in range(feats // GROUP_CH):
        at = slice(g * GROUP_CH, (g + 1) * GROUP_CH)
        pieces.append(
            lax.dot_general(
                x_ref[at, :], merge_ref[...], (((0,), (0,)), ((), ())), preferred_element_type=F32
            ).astype(BF16)
        )
    spectrum = jnp.concatenate(pieces, axis=1)
    part = width // OUT_PARTS
    copies = []
    for j in range(OUT_PARTS):
        at = slice(j * part, (j + 1) * part)
        out_v[:, at] = jnp.dot(spectrum, w_ref[:, at], preferred_element_type=F32).astype(BF16)
        copies.append(
            pltpu.make_async_copy(
                out_v.at[:, pl.ds(j * part, part)],
                out_hbm.at[0, :, pl.ds(j * part, part)],
                sems.at[j],
            )
        )
        copies[-1].start()
    for copy in copies:
        copy.wait()


VMEM = pl.BlockSpec(memory_space=pltpu.VMEM)
HBM = pl.BlockSpec(memory_space=pltpu.HBM)


def call_project(tokens, norm_gain, w_in, spread):
    _, toks, width = tokens.shape
    feats = w_in.shape[1]
    return pl.pallas_call(
        project,
        out_shape=pltpu.VMEM((feats, toks), BF16),
        in_specs=[HBM, HBM, HBM, HBM],
        out_specs=VMEM,
        scratch_shapes=[
            pltpu.VMEM((toks, width), BF16),
            pltpu.VMEM((width, feats), BF16),
            pltpu.VMEM(norm_gain.shape, BF16),
            pltpu.VMEM(spread.shape, BF16),
            pltpu.SemaphoreType.DMA((IN_PARTS,)),
            pltpu.SemaphoreType.DMA((3,)),
        ],
        compiler_params=pltpu.CompilerParams(vmem_limit_bytes=PROJECT_LIMIT),
        name="project",
    )(tokens, norm_gain, w_in, spread)


def call_transform_a(x, first, turn):
    half = jax.ShapeDtypeStruct((2 * CORES * x.shape[1], x.shape[1]), BF16)
    return pl.pallas_call(
        transform_a,
        out_shape=(half, half),
        in_specs=[VMEM, VMEM, VMEM],
        out_specs=(VMEM, VMEM),
        scratch_shapes=[pltpu.VMEM(x.shape, F32)],
        compiler_params=pltpu.CompilerParams(vmem_limit_bytes=VMEM_LIMIT),
        name="transform_a",
    )(x, first, turn)


def call_transform_b(own, got, last):
    shape = (CORES * last.shape[1], own.shape[1])
    return pl.pallas_call(
        transform_b,
        out_shape=jax.ShapeDtypeStruct(shape, BF16),
        in_specs=[VMEM, VMEM, VMEM],
        out_specs=VMEM,
        scratch_shapes=[pltpu.VMEM(shape, F32)],
        compiler_params=pltpu.CompilerParams(vmem_limit_bytes=VMEM_LIMIT),
        name="transform_b",
    )(own, got, last)


def call_merge_out(x, merge, w_out):
    width = w_out.shape[1]
    toks = x.shape[1]
    return pl.pallas_call(
        merge_out,
        out_shape=jax.ShapeDtypeStruct((1, toks, width), BF16),
        in_specs=[VMEM, VMEM, VMEM],
        out_specs=HBM,
        scratch_shapes=[pltpu.VMEM((toks, width), BF16), pltpu.SemaphoreType.DMA((OUT_PARTS,))],
        compiler_params=pltpu.CompilerParams(vmem_limit_bytes=VMEM_LIMIT),
        name="merge_out",
    )(x, merge, w_out)


def shards(rows, chips, tokens, norm_gain, w_in, w_out):
    _, toks, width = tokens.shape
    feats = w_in.shape[1]
    spread, merge = channel_tables()
    first, turn, last = sequence_tables(rows, chips, toks)

    def exchange(x):
        x = x.reshape(rows * chips, CORES, toks)
        x = lax.all_to_all(x, ("row", "y"), split_axis=0, concat_axis=0, tiled=True)
        return x.reshape(feats, toks)

    sent = exchange(call_project(tokens, norm_gain, w_in, jnp.asarray(spread, BF16)))
    own, give = call_transform_a(sent, jnp.asarray(first, BF16), jnp.asarray(turn, F32))
    got = lax.all_gather(give, "core")
    back = exchange(call_transform_b(own, got, jnp.asarray(last, BF16)))
    return call_merge_out(back, jnp.asarray(merge, BF16), w_out)


def solution(mesh):
    groups, rows, cols = (mesh.shape[name] for name in ("grp", "row", "col"))
    chips = cols // CORES
    split = jax.sharding.Mesh(
        mesh.devices.reshape(groups, rows, chips, CORES), ("grp", "row", "y", "core")
    )
    spec = P("grp", ("row", "y", "core"), None)
    return jax.shard_map(
        functools.partial(shards, rows, chips),
        mesh=split,
        in_specs=(spec, P(), P(), P()),
        out_specs=spec,
        check_vma=False,
    )
```

```python
import functools
import math

import jax
import jax.numpy as jnp
import numpy as np
from jax import lax
from jax.experimental import pallas as pl
from jax.experimental.pallas import tpu as pltpu
from jax.sharding import PartitionSpec as P

GROUP_CH = 128
NORM_EPS = 1e-06
CORES = 2
IN_PARTS = 4
OUT_SPLIT = (0, 6, 11, 15, 16)
VMEM_LIMIT = 16 * 1024 * 1024
PROJECT_LIMIT = 60 * 1024 * 1024

BF16 = jnp.bfloat16
F32 = jnp.float32


def channel_tables():
    half = GROUP_CH // 2
    q = np.arange(GROUP_CH)[:, None]
    f = np.arange(GROUP_CH)[None, :]
    freq = np.where(f <= half, f, GROUP_CH - f)
    angle = 2.0 * np.pi * (q * freq % GROUP_CH) / GROUP_CH
    spread = np.where(f <= half, np.cos(angle), np.sin(angle))
    merge = np.zeros((GROUP_CH, GROUP_CH))
    merge[0, 0] = merge[half, half] = 1.0
    for m in range(1, half):
        merge[m, m] = merge[m, GROUP_CH - m] = 1.0
        merge[GROUP_CH - m, m] = -1.0
        merge[GROUP_CH - m, GROUP_CH - m] = 1.0
    return spread, merge


def sequence_tables(rows, chips, toks):
    length = rows * chips * CORES * toks
    low = CORES * toks
    high = rows * chips
    assert high == low
    a = np.arange(high)
    b = np.arange(low)
    first = 2.0 * np.pi * (a[:, None] * a[None, :] % high) / high
    turn = 2.0 * np.pi * (b[:, None] * a[None, :] % length) / length
    last = 2.0 * np.pi * (a[:, None] * b[None, :] % low) / low
    scale = 1.0 / math.sqrt(length * GROUP_CH)
    spread = np.zeros((high, CORES, 2, toks))
    gather = np.zeros((CORES, high, 2, toks))
    turns = np.zeros((CORES, CORES, 2, toks, toks))
    for h in range(CORES):
        at = slice(h * toks, (h + 1) * toks)
        spread[:, h, 0] = np.cos(first[:, at])
        spread[:, h, 1] = -np.sin(first[:, at])
        gather[h, :, 0] = np.cos(last[:, at])
        gather[h, :, 1] = np.sin(last[:, at])
        for c in range(CORES):
            angle = turn[c * toks : (c + 1) * toks, at]
            turns[c, h, 0] = np.cos(angle) * scale
            turns[c, h, 1] = -np.sin(angle) * scale
    return spread.reshape(high, -1), turns, gather.reshape(CORES, high, -1)


def project(
    tok_hbm, gain_hbm, w_hbm, spread_hbm, out_ref, tok_v, w_v, gain_v, spread_v, w_sems, sems
):
    toks, width = tok_v.shape
    part = width // IN_PARTS
    tok_copy = pltpu.make_async_copy(tok_hbm.at[0], tok_v, sems.at[0])
    gain_copy = pltpu.make_async_copy(gain_hbm, gain_v, sems.at[1])
    spread_copy = pltpu.make_async_copy(spread_hbm, spread_v, sems.at[2])
    w_copies = []
    for j in range(IN_PARTS):
        at = pl.ds(j * part, part)
        w_copies.append(pltpu.make_async_copy(w_hbm.at[at, :], w_v.at[at, :], w_sems.at[j]))
    for copy in [tok_copy, gain_copy, *w_copies, spread_copy]:
        copy.start()
    tok_copy.wait()
    gain_copy.wait()
    x = tok_v[...].astype(F32)
    gain = gain_v[...].astype(F32).reshape(1, width)
    factor = lax.rsqrt(jnp.mean(x * x, axis=-1, keepdims=True) + NORM_EPS)
    tok_v[...] = (x * gain).astype(BF16)
    total = jnp.zeros((toks, w_v.shape[1]), F32)
    for j in range(IN_PARTS):
        at = slice(j * part, (j + 1) * part)
        w_copies[j].wait()
        total += jnp.dot(tok_v[:, at], w_v[at, :], preferred_element_type=F32)
    mixin = (total * factor).astype(BF16)
    spread_copy.wait()
    for g in range(w_v.shape[1] // GROUP_CH):
        at = slice(g * GROUP_CH, (g + 1) * GROUP_CH)
        out_ref[at, :] = lax.dot_general(
            spread_v[...], mixin[:, at], (((0,), (1,)), ((), ())), preferred_element_type=F32
        ).astype(BF16)


def transform_a(x_ref, first_ref, turn_ref, own_ref, send_ref, wide):
    count, toks = x_ref.shape
    wide[...] = x_ref[...].astype(F32)
    core = lax.axis_index("core")
    feature = (lax.axis_index("row") * lax.axis_size("y") + lax.axis_index("y")) * CORES
    low = core == 0
    for j in range(CORES):
        x = wide[pl.ds(j, count // CORES, stride=CORES), :].astype(BF16)
        y = lax.dot_general(
            x, first_ref[...], (((0,), (0,)), ((), ())), preferred_element_type=F32
        )
        sine = lax.rem(feature + j, GROUP_CH) > GROUP_CH // 2
        halves = []
        for h in range(CORES):
            at = 2 * h * toks
            y_re, y_im = y[:, at : at + toks], y[:, at + toks : at + 2 * toks]
            w_re, w_im = turn_ref[core, h, 0], turn_ref[core, h, 1]
            u_re = (y_re * w_re - y_im * w_im).astype(BF16)
            u_im = (y_re * w_im + y_im * w_re).astype(BF16)
            halves.append((jnp.where(sine, -u_im, u_re), jnp.where(sine, u_re, u_im)))
        for k in range(2):
            part = slice((2 * j + k) * toks, (2 * j + k + 1) * toks)
            own_ref[part, :] = jnp.where(low, halves[0][k], halves[1][k])
            send_ref[part, :] = jnp.where(low, halves[1][k], halves[0][k])


def transform_b(own_ref, got_ref, last_ref, out_ref, wide):
    core = lax.axis_index("core")
    count = wide.shape[0] // CORES
    part = own_ref.shape[0] // CORES
    for j in range(CORES):
        at = slice(j * part, (j + 1) * part)
        z = jnp.dot(last_ref[core], own_ref[at, :], preferred_element_type=F32)
        z += jnp.dot(last_ref[1 - core], got_ref[1 - core, at, :], preferred_element_type=F32)
        wide[pl.ds(j, count, stride=CORES), :] = z
    out_ref[...] = wide[...].astype(BF16)


def merge_out(x_ref, merge_ref, w_ref, out_hbm, out_v, sems):
    feats = x_ref.shape[0]
    width = w_ref.shape[1]
    pieces = []
    for g in range(feats // GROUP_CH):
        at = slice(g * GROUP_CH, (g + 1) * GROUP_CH)
        pieces.append(
            lax.dot_general(
                x_ref[at, :], merge_ref[...], (((0,), (0,)), ((), ())), preferred_element_type=F32
            ).astype(BF16)
        )
    spectrum = jnp.concatenate(pieces, axis=1)
    copies = []
    for j in range(len(OUT_SPLIT) - 1):
        low, high = (width * cut // OUT_SPLIT[-1] for cut in OUT_SPLIT[j : j + 2])
        out_v[:, low:high] = jnp.dot(
            spectrum, w_ref[:, low:high], preferred_element_type=F32
        ).astype(BF16)
        at = pl.ds(low, high - low)
        copies.append(pltpu.make_async_copy(out_v.at[:, at], out_hbm.at[0, :, at], sems.at[j]))
        copies[-1].start()
    for copy in copies:
        copy.wait()


VMEM = pl.BlockSpec(memory_space=pltpu.VMEM)
HBM = pl.BlockSpec(memory_space=pltpu.HBM)


def call_project(tokens, norm_gain, w_in, spread):
    _, toks, width = tokens.shape
    feats = w_in.shape[1]
    return pl.pallas_call(
        project,
        out_shape=pltpu.VMEM((feats, toks), BF16),
        in_specs=[HBM, HBM, HBM, HBM],
        out_specs=VMEM,
        scratch_shapes=[
            pltpu.VMEM((toks, width), BF16),
            pltpu.VMEM((width, feats), BF16),
            pltpu.VMEM(norm_gain.shape, BF16),
            pltpu.VMEM(spread.shape, BF16),
            pltpu.SemaphoreType.DMA((IN_PARTS,)),
            pltpu.SemaphoreType.DMA((3,)),
        ],
        compiler_params=pltpu.CompilerParams(vmem_limit_bytes=PROJECT_LIMIT),
        name="project",
    )(tokens, norm_gain, w_in, spread)


def call_transform_a(x, first, turn):
    half = jax.ShapeDtypeStruct((2 * CORES * x.shape[1], x.shape[1]), BF16)
    return pl.pallas_call(
        transform_a,
        out_shape=(half, half),
        in_specs=[VMEM, VMEM, VMEM],
        out_specs=(VMEM, VMEM),
        scratch_shapes=[pltpu.VMEM(x.shape, F32)],
        compiler_params=pltpu.CompilerParams(vmem_limit_bytes=VMEM_LIMIT),
        name="transform_a",
    )(x, first, turn)


def call_transform_b(own, got, last):
    shape = (CORES * last.shape[1], own.shape[1])
    return pl.pallas_call(
        transform_b,
        out_shape=jax.ShapeDtypeStruct(shape, BF16),
        in_specs=[VMEM, VMEM, VMEM],
        out_specs=VMEM,
        scratch_shapes=[pltpu.VMEM(shape, F32)],
        compiler_params=pltpu.CompilerParams(vmem_limit_bytes=VMEM_LIMIT),
        name="transform_b",
    )(own, got, last)


def call_merge_out(x, merge, w_out):
    width = w_out.shape[1]
    toks = x.shape[1]
    return pl.pallas_call(
        merge_out,
        out_shape=jax.ShapeDtypeStruct((1, toks, width), BF16),
        in_specs=[VMEM, VMEM, VMEM],
        out_specs=HBM,
        scratch_shapes=[pltpu.VMEM((toks, width), BF16), pltpu.SemaphoreType.DMA((len(OUT_SPLIT) - 1,))],
        compiler_params=pltpu.CompilerParams(vmem_limit_bytes=VMEM_LIMIT),
        name="merge_out",
    )(x, merge, w_out)


def shards(rows, chips, tokens, norm_gain, w_in, w_out):
    _, toks, width = tokens.shape
    feats = w_in.shape[1]
    spread, merge = channel_tables()
    first, turn, last = sequence_tables(rows, chips, toks)

    def exchange(x):
        x = x.reshape(rows * chips, CORES, toks)
        x = lax.all_to_all(x, ("row", "y"), split_axis=0, concat_axis=0, tiled=True)
        return x.reshape(feats, toks)

    sent = exchange(call_project(tokens, norm_gain, w_in, jnp.asarray(spread, BF16)))
    own, give = call_transform_a(sent, jnp.asarray(first, BF16), jnp.asarray(turn, F32))
    got = lax.all_gather(give, "core")
    back = exchange(call_transform_b(own, got, jnp.asarray(last, BF16)))
    return call_merge_out(back, jnp.asarray(merge, BF16), w_out)


def solution(mesh):
    groups, rows, cols = (mesh.shape[name] for name in ("grp", "row", "col"))
    chips = cols // CORES
    split = jax.sharding.Mesh(
        mesh.devices.reshape(groups, rows, chips, CORES), ("grp", "row", "y", "core")
    )
    spec = P("grp", ("row", "y", "core"), None)
    return jax.shard_map(
        functools.partial(shards, rows, chips),
        mesh=split,
        in_specs=(spec, P(), P(), P()),
        out_specs=spec,
        check_vma=False,
    )
```
